32 devices in a mesh: ep: 4 (over y, x), tp: 8 (over z, core).
Axes of the slice: x: 2, y: 2, z: 4, core: 2. Of those that a mesh axis runs over, the one named last changes fastest.
Arguments:
- tokens: bfloat16 [128, 2048], P('ep'), may hold values from -6 to 6
- norm_gain: float32 [2048], replicated, may hold values from 0.1 to 1.9
- routes: int32 [128, 2], P('ep'), may hold values from 0 to 3, all different within a row; in each aligned block of 32 rows (0 to 31, 32 to 63, ...) at most 16 rows name the same one
- gate_weights: float32 [128, 2], P('ep'), may hold values from 0.1 to 1
- expert_gate: bfloat16 [4, 2048, 8192], P('ep', None, 'tp'), may hold values from -0.125 to 0.125
- expert_up: bfloat16 [4, 2048, 8192], P('ep', None, 'tp'), may hold values from -0.125 to 0.125
- expert_down: bfloat16 [4, 8192, 2048], P('ep', 'tp'), may hold values from -0.0625 to 0.0625
Outputs:
- mixed: bfloat16 [128, 2048], P('ep', 'tp')
The draws below stay inside these ranges and needn't reach their ends.
Inputs may be any that keep to these rules, and one draw needn't show every extreme that they name: `routes`: each row names 2 different experts; among the rows of one index of ep no expert is named by more than 16 rows.
All inputs are finite; a program needn't handle non-finite values.
Results may differ from the reference program's by a relative error of at most 0.0095.
Values may be sent and summed in bfloat16 or wider, within the bound.
A program may use at most 64 MiB of HBM per device.

```python
import math
import jax
import jax.numpy as jnp
import numpy as np
from jax import lax

D = 2048
FF = 8192
TOP = 2
TOK_DEV = 32
EXPERTS = 4
CAP = 16
TOKENS = 128


def shard_levels(rng, shape, pieces, low, high):
    def one(position, blocks):
        steps = jax.random.uniform(jax.random.fold_in(jax.random.fold_in(rng, 6), position), (blocks,), jnp.float32, low / len(pieces), high / len(pieces))
        return jnp.repeat(jnp.exp(steps), shape[position] // blocks).reshape((-1,) + (1,) * (len(shape) - position - 1))

    gain = one(*pieces[0])
    for cut in pieces[1:]:
        gain = gain * one(*cut)
    return gain


def routed_block(key, own, number, rows, count, top, limit, slope):
    order = jax.random.permutation(key, count)
    heavy_load, common = portions_of(count, rows * top, limit, slope, True), portions_of(count, rows * top, limit, slope, False)
    places = jnp.arange(count)

    def named(tallies, offset_by):
        used = int((tallies > 0).sum())
        fixed = max(1, used // 4)
        shifted = fixed + (places - fixed + offset_by * (used - fixed)) % max(1, count - fixed)
        return jnp.zeros((count,), jnp.int32).at[order[jnp.where(places < fixed, places, shifted)]].set(jnp.asarray(tallies, jnp.int32))

    tallies = jnp.where(number % 4 == 0, named(heavy_load, number // 4), named(common, number - number // 4 - 1))
    mixed = jax.random.permutation(jax.random.fold_in(own, 3), count)
    giver, taker = mixed[0:count // 2 * 2:2], mixed[1:count // 2 * 2:2]
    room = jnp.minimum(tallies[giver] - 1, limit - tallies[taker]) // 2
    room = jnp.where((giver == order[0]) | (taker == order[0]) | (tallies[taker] == 0), 0, jnp.maximum(room, 0))
    shifted = jax.random.randint(jax.random.fold_in(own, 4), (count // 2,), 0, 1 << 20) % (room + 1)
    tallies = tallies.at[giver].add(-shifted).at[taker].add(shifted)
    members = jnp.searchsorted(jnp.cumsum(tallies), jnp.arange(rows * top), side="right").astype(jnp.int32)
    table = members.reshape(top, rows).T
    table = table[jax.random.permutation(jax.random.fold_in(own, 1), rows)]
    offset_by = jax.random.randint(jax.random.fold_in(own, 2), (rows, 1), 0, top)
    return jnp.take_along_axis(table, (jnp.arange(top)[None, :] + offset_by) % top, axis=1)


def portions_of(number_of, total, most, lean, full):
    weights = [(1 << 20) // math.isqrt(grade ** lean) + 1 for grade in range(1, number_of + 1)]
    largest = most if full else min(most, max(-(-total // number_of), total * weights[0] // sum(weights)))
    least = 1 if total - largest >= number_of - 1 else 0
    holding, spare = [largest] + [least] * (number_of - 1), total - largest - least * (number_of - 1)
    while spare > 0:
        free = [i for i in range(1, number_of) if holding[i] < largest] or [i for i in range(1, number_of) if holding[i] < most]
        mass, left = sum([weights[i] for i in free]), spare
        for i in free:
            extra = min(most - holding[i], max(1, left * weights[i] // mass), spare)
            holding[i] = holding[i] + extra
            spare = spare - extra
    return np.array(holding)


def noise(key, shape, width, most, shards=(), kind=jnp.bfloat16):
    entries = jax.random.normal(key, shape, jnp.float32) * width
    if len(shards) > 0:
        entries = shard_levels(key, shape, shards, -0.22, 0.18) * entries
    return jnp.clip(entries, min=-most, max=most).astype(kind)


def setup_inputs(seed: int = 0) -> dict:
    key_list = jax.random.split(jax.random.key(seed), 8)
    tokens = noise(key_list[0], (TOKENS, D), 1.0, 6.0, ((0, 4),))
    norm_gain = jnp.clip(1.0 + 0.18 * jax.random.normal(key_list[1], (D,), jnp.float32), 0.1, 1.9)
    routes_keys = jax.random.split(jax.random.fold_in(key_list[2], 1), TOKENS // TOK_DEV)
    routes_turns = jax.random.permutation(jax.random.fold_in(key_list[2], 3), TOKENS // TOK_DEV)
    routes = jax.vmap(lambda own, number: routed_block(jax.random.fold_in(key_list[2], 2), own, number, TOK_DEV, EXPERTS, TOP, CAP, 2))(routes_keys, routes_turns).reshape((TOKENS, TOP))
    gate_weights = jnp.clip(0.1 + 0.9 * jax.random.uniform(key_list[3], (TOKENS, TOP), jnp.float32) ** shard_levels(key_list[3], (TOKENS, TOP), ((0, 4),), -0.2, 0.2), 0.1, 1.0)
    expert_gate = noise(key_list[4], (EXPERTS, D, FF), D ** -0.5, 0.125, ((0, 4), (2, 8)))
    expert_up = noise(key_list[5], (EXPERTS, D, FF), D ** -0.5, 0.125, ((0, 4), (2, 8)))
    expert_down = noise(key_list[6], (EXPERTS, FF, D), FF ** -0.5, 0.0625, ((0, 4), (1, 8)))
    return {"tokens": tokens, "norm_gain": norm_gain, "routes": routes, "gate_weights": gate_weights, "expert_gate": expert_gate, "expert_up": expert_up, "expert_down": expert_down}


def reference(tokens, norm_gain, routes, gate_weights, expert_gate, expert_up, expert_down):
    values = tokens.astype(jnp.float32)
    scale = lax.rsqrt(lax.optimization_barrier(jnp.mean(values * values, axis=-1, keepdims=True)) + 1e-06)
    normed = (values * scale * norm_gain[None, :]).astype(jnp.bfloat16)
    chosen = (routes[:, :, None] == jnp.arange(EXPERTS, dtype=jnp.int32)[None, None, :]).astype(jnp.float32)
    coefs = lax.optimization_barrier(jnp.sum(gate_weights[:, :, None] * chosen, axis=1))

    def expert_step(total, packed):
        w_gate, w_up, w_down, weight = packed
        gate = jnp.dot(normed, w_gate, preferred_element_type=jnp.float32)
        upper = jnp.dot(normed, w_up, preferred_element_type=jnp.float32)
        hidden = (jax.nn.silu(gate) * upper).astype(jnp.bfloat16)
        output = jnp.dot(hidden, w_down, preferred_element_type=jnp.float32)
        return (total + weight[:, None] * output, None)
    start = jnp.zeros((tokens.shape[0], tokens.shape[1]), jnp.float32)
    total, _ = lax.scan(expert_step, start, (expert_gate, expert_up, expert_down, coefs.T))
    return total.astype(jnp.bfloat16)
```

```python
import functools

import jax
import jax.numpy as jnp
from jax import lax
from jax.experimental import pallas as pl
from jax.experimental.pallas import tpu as pltpu
from jax.sharding import PartitionSpec as P

MESH = pl.DeviceIdType.MESH


def expert_rows(rows, w_gate, w_up):
    gate = jnp.dot(rows, w_gate, preferred_element_type=jnp.float32)
    upper = jnp.dot(rows, w_up, preferred_element_type=jnp.float32)
    return (jax.nn.silu(gate) * upper).astype(jnp.bfloat16)


def shards(tokens, norm_gain, routes, gate_weights, expert_gate, expert_up, expert_down):
    tok_rows, width = tokens.shape
    n_ep = lax.axis_size("ep")
    n_tp = lax.axis_size("tp")
    part_width = width // n_tp
    values = tokens.astype(jnp.float32)
    scale = lax.rsqrt(jnp.mean(values * values, axis=-1, keepdims=True) + 1e-06)
    normed = (values * scale * norm_gain[None, :]).astype(jnp.bfloat16)
    w_gate = expert_gate[0]
    w_up = expert_up[0]
    w_down = expert_down[0]
    capacity = tok_rows // 2
    picks = routes.reshape(-1)
    chosen = (picks[:, None] == jnp.arange(n_ep, dtype=jnp.int32)[None, :]).astype(jnp.int32)
    ranks = jnp.cumsum(chosen, axis=0) - chosen
    place = picks * capacity + jnp.sum(ranks * chosen, axis=1)
    table = (place[None, :] == jnp.arange(n_ep * capacity, dtype=jnp.int32)[:, None]).astype(
        jnp.float32
    )
    slots = jnp.sum(table.reshape(n_ep * capacity, tok_rows, 2), axis=2)
    buffer = jnp.dot(slots.astype(jnp.bfloat16), normed, preferred_element_type=jnp.float32)
    buffer = buffer.astype(jnp.bfloat16).reshape(n_ep, capacity, width)
    combine = jnp.sum(
        (table * gate_weights.reshape(-1)[None, :]).reshape(n_ep * capacity, tok_rows, 2), axis=2
    ).T
    received = lax.all_to_all(buffer, "ep", split_axis=0, concat_axis=0, tiled=True)
    sources = received.shape[0]
    count = received.shape[1]
    hidden = expert_rows(received.reshape(sources * count, width), w_gate, w_up)
    partial_value = jnp.dot(hidden, w_down, preferred_element_type=jnp.float32)
    outputs = lax.psum_scatter(
        partial_value.reshape(sources, count, width), "tp", scatter_dimension=2, tiled=True
    )
    back = lax.all_to_all(outputs, "ep", split_axis=0, concat_axis=0, tiled=True)
    mixed = jnp.dot(
        combine,
        back.reshape(n_ep * capacity, part_width),
        precision=lax.Precision.HIGHEST,
        preferred_element_type=jnp.float32,
    )
    return mixed.astype(jnp.bfloat16)


def step_kernel(n_ep, n_z, cap, nk, tok_hbm, gain_ref, routes_ref, gw_ref, wg_hbm, wu_hbm, wd_hbm,
                out_ref, tok, wg, wu, wd, sendbuf, recv, acc_g, acc_u, hid, pbuf, prbuf, obuf, fin,
                tok_sem, wg_sem, wu_sem, wd_sem, d_send, d_recv, p_send, p_recv, f_send, f_recv):
    me = lax.axis_index("ep")
    t = lax.axis_index("tp")
    z = t // 2
    c = t % 2
    other = 1 - c
    partner = 2 * z + other
    rows, width = tok.shape
    ff = wg.shape[1]
    kc = width // nk
    pw = out_ref.shape[1]
    slots_n = n_ep * cap

    tok_copy = pltpu.make_async_copy(tok_hbm, tok, tok_sem)
    tok_copy.start()

    barrier = pltpu.get_barrier_semaphore()
    pl.semaphore_signal(barrier, inc=1, device_id=(me, partner), device_id_type=MESH)
    for dz in range(n_z):
        for ds in range(n_ep):
            if dz or ds:
                dest = (lax.rem(me + ds, n_ep), 2 * lax.rem(z + dz, n_z) + c)
                pl.semaphore_signal(barrier, inc=1, device_id=dest, device_id_type=MESH)

    w_copies = []
    for k in range(nk):
        cut = pl.ds(k * kc, kc)
        cg = pltpu.make_async_copy(wg_hbm.at[0, cut], wg.at[cut], wg_sem.at[k])
        cu = pltpu.make_async_copy(wu_hbm.at[0, cut], wu.at[cut], wu_sem.at[k])
        cg.start()
        cu.start()
        w_copies.append((cg, cu))
    d_copy = pltpu.make_async_copy(wd_hbm.at[0], wd, wd_sem)
    d_copy.start()

    shape3 = (n_ep, cap, rows)
    expert = lax.broadcasted_iota(jnp.int32, shape3, 0).reshape(slots_n, rows)
    slot = lax.broadcasted_iota(jnp.int32, shape3, 1).reshape(slots_n, rows)
    first = routes_ref[0:1, :] == expert
    second = routes_ref[1:2, :] == expert
    chosen = jnp.where(first | second, 1.0, 0.0)
    before = jnp.where(
        lax.broadcasted_iota(jnp.int32, (rows, rows), 0)
        < lax.broadcasted_iota(jnp.int32, (rows, rows), 1), 1.0, 0.0)
    rank = jnp.dot(chosen.astype(jnp.bfloat16), before.astype(jnp.bfloat16),
                   preferred_element_type=jnp.float32)
    table = jnp.where(rank == slot.astype(jnp.float32), chosen, 0.0)
    weight = jnp.where(first, gw_ref[0:1, :], 0.0) + jnp.where(second, gw_ref[1:2, :], 0.0)
    combine = (table * weight).T
    table = table.astype(jnp.bfloat16)

    tok_copy.wait()
    values = tok[...].astype(jnp.float32)
    scale = lax.rsqrt(jnp.mean(values * values, axis=-1, keepdims=True) + 1e-06)
    for k in range(nk):
        cut = slice(k * kc, (k + 1) * kc)
        normed = (tok[:, cut].astype(jnp.float32) * scale * gain_ref[:, cut]).astype(jnp.bfloat16)
        block = jnp.dot(table, normed, preferred_element_type=jnp.float32).astype(jnp.bfloat16)
        sendbuf[k] = block.reshape(n_ep, cap, kc)
    for k in range(nk):
        recv[k, me] = sendbuf[k, me]

    pl.semaphore_wait(barrier, n_z * n_ep)

    dispatch = []
    for k in range(nk):
        per = []
        for i in range(1, n_ep):
            dest = lax.rem(me + i, n_ep)
            copy = pltpu.make_async_remote_copy(
                src_ref=sendbuf.at[k, dest], dst_ref=recv.at[k, me],
                send_sem=d_send.at[k, i - 1], recv_sem=d_recv.at[k, i - 1],
                device_id=(dest, t), device_id_type=MESH)
            copy.start()
            per.append(copy)
        dispatch.append(per)

    for k in range(nk):
        w_copies[k][0].wait()
        w_copies[k][1].wait()
        for copy in dispatch[k]:
            copy.wait_recv()
        x = recv[k].reshape(slots_n, kc)
        g = jnp.dot(x, wg[k * kc:(k + 1) * kc, :], preferred_element_type=jnp.float32)
        u = jnp.dot(x, wu[k * kc:(k + 1) * kc, :], preferred_element_type=jnp.float32)
        if k == 0:
            acc_g[...] = g
            acc_u[...] = u
        elif k < nk - 1:
            acc_g[...] += g
            acc_u[...] += u
        else:
            g = acc_g[...] + g
            u = acc_u[...] + u
            hid[...] = (g / (1.0 + jnp.exp(-g)) * u).astype(jnp.bfloat16)

    d_copy.wait()
    order = sorted(range(n_z), key=lambda d: -min(d, n_z - d))
    crossing = []
    for j, dz in enumerate(order):
        zz = lax.rem(z + dz, n_z)
        cut = pl.ds(pl.multiple_of((2 * zz + other) * pw, 128), pw)
        pbuf[j] = jnp.dot(hid[...], wd[:, cut], preferred_element_type=jnp.float32)
        copy = pltpu.make_async_remote_copy(
            src_ref=pbuf.at[j], dst_ref=prbuf.at[j], send_sem=p_send.at[j], recv_sem=p_recv.at[j],
            device_id=(me, partner), device_id_type=MESH)
        copy.start()
        crossing.append(copy)
    final = []
    for j, dz in enumerate(order):
        zz = lax.rem(z + dz, n_z)
        cut = pl.ds(pl.multiple_of((2 * zz + c) * pw, 128), pw)
        own = jnp.dot(hid[...], wd[:, cut], preferred_element_type=jnp.float32)
        crossing[j].wait_recv()
        block = (own + prbuf[j]).astype(jnp.bfloat16).reshape(n_ep, cap, pw)
        obuf[j] = block
        for ds in range(n_ep):
            dest = lax.rem(me + ds, n_ep)
            if dz or ds:
                copy = pltpu.make_async_remote_copy(
                    src_ref=obuf.at[j, dest], dst_ref=fin.at[z, me],
                    send_sem=f_send.at[j, ds], recv_sem=f_recv.at[j, ds],
                    device_id=(dest, 2 * zz + c), device_id_type=MESH)
                copy.start()
                final.append(copy)
            else:
                fin[z, me] = obuf[j, me]

    for per in dispatch:
        for copy in per:
            copy.wait_send()
    for copy in crossing:
        copy.wait_send()
    for copy in final:
        copy.wait_recv()
    total = fin[0].astype(jnp.float32)
    for i in range(1, n_z):
        total = total + fin[i].astype(jnp.float32)
    mixed = jnp.dot(combine, total.reshape(slots_n, pw), precision=lax.Precision.HIGHEST,
                    preferred_element_type=jnp.float32)
    out_ref[...] = mixed.astype(jnp.bfloat16)
    for copy in final:
        copy.wait_send()


def fused(tokens, norm_gain, routes, gate_weights, expert_gate, expert_up, expert_down):
    rows, width = tokens.shape
    n_ep = lax.axis_size("ep")
    n_tp = lax.axis_size("tp")
    n_z = n_tp // 2
    pw = width // n_tp
    cap = rows // 2
    ff = expert_gate.shape[2]
    slots_n = n_ep * cap
    nk = 4
    kc = width // nk
    vmem = pl.BlockSpec(memory_space=pltpu.VMEM)
    hbm = pl.BlockSpec(memory_space=pl.ANY)
    bf, f32 = jnp.bfloat16, jnp.float32
    dma = pltpu.SemaphoreType.DMA
    return pl.pallas_call(
        functools.partial(step_kernel, n_ep, n_z, cap, nk),
        out_shape=jax.ShapeDtypeStruct((rows, pw), bf),
        in_specs=[hbm, vmem, vmem, vmem, hbm, hbm, hbm],
        out_specs=vmem,
        scratch_shapes=[
            pltpu.VMEM((rows, width), bf),
            pltpu.VMEM((width, ff), bf),
            pltpu.VMEM((width, ff), bf),
            pltpu.VMEM((ff, width), bf),
            pltpu.VMEM((nk, n_ep, cap, kc), bf),
            pltpu.VMEM((nk, n_ep, cap, kc), bf),
            pltpu.VMEM((slots_n, ff), f32),
            pltpu.VMEM((slots_n, ff), f32),
            pltpu.VMEM((slots_n, ff), bf),
            pltpu.VMEM((n_z, slots_n, pw), f32),
            pltpu.VMEM((n_z, slots_n, pw), f32),
            pltpu.VMEM((n_z, n_ep, cap, pw), bf),
            pltpu.VMEM((n_z, n_ep, cap, pw), bf),
            dma, dma((nk,)), dma((nk,)), dma,
            dma((nk, n_ep - 1)), dma((nk, n_ep - 1)),
            dma((n_z,)), dma((n_z,)),
            dma((n_z, n_ep)), dma((n_z, n_ep)),
        ],
        compiler_params=pltpu.CompilerParams(
            collective_id=0, has_side_effects=True, vmem_limit_bytes=60 * 1024 * 1024),
    )(tokens, norm_gain.reshape(1, width), routes.T, gate_weights.T, expert_gate, expert_up,
      expert_down)


def body(tokens, *rest):
    rows, width = tokens.shape
    n_tp = lax.axis_size("tp")
    if n_tp % 2 == 0 and (width // n_tp) % 128 == 0 and rows % 32 == 0:
        return fused(tokens, *rest)
    return shards(tokens, *rest)


def solution(mesh):
    placed = (
        P("ep", None),
        P(),
        P("ep", None),
        P("ep", None),
        P("ep", None, "tp"),
        P("ep", None, "tp"),
        P("ep", "tp", None),
    )
    return jax.shard_map(
        body, mesh=mesh, in_specs=placed, out_specs=P("ep", "tp"), check_vma=False
    )
```

```python
import functools

import jax
import jax.numpy as jnp
from jax import lax
from jax.experimental import pallas as pl
from jax.experimental.pallas import tpu as pltpu
from jax.sharding import PartitionSpec as P

MESH = pl.DeviceIdType.MESH


def expert_rows(rows, w_gate, w_up):
    gate = jnp.dot(rows, w_gate, preferred_element_type=jnp.float32)
    upper = jnp.dot(rows, w_up, preferred_element_type=jnp.float32)
    return (jax.nn.silu(gate) * upper).astype(jnp.bfloat16)


def shards(tokens, norm_gain, routes, gate_weights, expert_gate, expert_up, expert_down):
    tok_rows, width = tokens.shape
    n_ep = lax.axis_size("ep")
    n_tp = lax.axis_size("tp")
    part_width = width // n_tp
    values = tokens.astype(jnp.float32)
    scale = lax.rsqrt(jnp.mean(values * values, axis=-1, keepdims=True) + 1e-06)
    normed = (values * scale * norm_gain[None, :]).astype(jnp.bfloat16)
    w_gate = expert_gate[0]
    w_up = expert_up[0]
    w_down = expert_down[0]
    capacity = tok_rows // 2
    picks = routes.reshape(-1)
    chosen = (picks[:, None] == jnp.arange(n_ep, dtype=jnp.int32)[None, :]).astype(jnp.int32)
    ranks = jnp.cumsum(chosen, axis=0) - chosen
    place = picks * capacity + jnp.sum(ranks * chosen, axis=1)
    table = (place[None, :] == jnp.arange(n_ep * capacity, dtype=jnp.int32)[:, None]).astype(
        jnp.float32
    )
    slots = jnp.sum(table.reshape(n_ep * capacity, tok_rows, 2), axis=2)
    buffer = jnp.dot(slots.astype(jnp.bfloat16), normed, preferred_element_type=jnp.float32)
    buffer = buffer.astype(jnp.bfloat16).reshape(n_ep, capacity, width)
    combine = jnp.sum(
        (table * gate_weights.reshape(-1)[None, :]).reshape(n_ep * capacity, tok_rows, 2), axis=2
    ).T
    received = lax.all_to_all(buffer, "ep", split_axis=0, concat_axis=0, tiled=True)
    sources = received.shape[0]
    count = received.shape[1]
    hidden = expert_rows(received.reshape(sources * count, width), w_gate, w_up)
    partial_value = jnp.dot(hidden, w_down, preferred_element_type=jnp.float32)
    outputs = lax.psum_scatter(
        partial_value.reshape(sources, count, width), "tp", scatter_dimension=2, tiled=True
    )
    back = lax.all_to_all(outputs, "ep", split_axis=0, concat_axis=0, tiled=True)
    mixed = jnp.dot(
        combine,
        back.reshape(n_ep * capacity, part_width),
        precision=lax.Precision.HIGHEST,
        preferred_element_type=jnp.float32,
    )
    return mixed.astype(jnp.bfloat16)


def step_kernel(n_ep, n_z, cap, nk, tok_hbm, gain_hbm, routes_hbm, gw_hbm, wg_hbm, wu_hbm, wd_hbm,
                out_ref, tok, gain_ref, routes_ref, gw_ref, wg, wu, wd, sendbuf, recv, acc_g, acc_u,
                hid, pbuf, prbuf, obuf, fin, tok_sem, small_sem, wg_sem, wu_sem, wd_sem, d_send,
                d_recv, p_send, p_recv, f_send, f_recv, line_sem):
    me = lax.axis_index("ep")
    t = lax.axis_index("tp")
    z = t // 2
    c = t % 2
    other = 1 - c
    partner = 2 * z + other
    rows, width = tok.shape
    kc = width // nk
    pw = out_ref.shape[1]
    slots_n = n_ep * cap
    above = z < n_z - 1
    below = z > 0

    tok_copy = pltpu.make_async_copy(tok_hbm, tok, tok_sem)
    tok_copy.start()

    barrier = pltpu.get_barrier_semaphore()
    for i in range(1, n_ep):
        pl.semaphore_signal(barrier, inc=1, device_id=(lax.rem(me + i, n_ep), t),
                            device_id_type=MESH)
    pl.semaphore_signal(barrier, inc=1, device_id=(me, partner), device_id_type=MESH)

    @pl.when(above)
    def _():
        pl.semaphore_signal(barrier, inc=1, device_id=(me, t + 2), device_id_type=MESH)

    @pl.when(below)
    def _():
        pl.semaphore_signal(barrier, inc=1, device_id=(me, t - 2), device_id_type=MESH)

    def line_signal(r):
        @pl.when(above)
        def _():
            pl.semaphore_signal(line_sem.at[r, 0], inc=1, device_id=(me, t + 2),
                                device_id_type=MESH)

        @pl.when(below)
        def _():
            pl.semaphore_signal(line_sem.at[r, 1], inc=1, device_id=(me, t - 2),
                                device_id_type=MESH)

    def line_wait(r):
        @pl.when(below)
        def _():
            pl.semaphore_wait(line_sem.at[r, 0], 1)

        @pl.when(above)
        def _():
            pl.semaphore_wait(line_sem.at[r, 1], 1)

    small = [pltpu.make_async_copy(routes_hbm, routes_ref, small_sem.at[0]),
             pltpu.make_async_copy(gw_hbm, gw_ref, small_sem.at[1]),
             pltpu.make_async_copy(gain_hbm, gain_ref, small_sem.at[2])]
    for copy in small:
        copy.start()

    w_copies = []
    for k in range(nk):
        cut = pl.ds(k * kc, kc)
        cg = pltpu.make_async_copy(wg_hbm.at[0, cut], wg.at[cut], wg_sem.at[k])
        cu = pltpu.make_async_copy(wu_hbm.at[0, cut], wu.at[cut], wu_sem.at[k])
        cg.start()
        cu.start()
        w_copies.append((cg, cu))
    d_copy = pltpu.make_async_copy(wd_hbm.at[0], wd, wd_sem)
    d_copy.start()

    small[0].wait()
    small[1].wait()
    shape3 = (n_ep, cap, rows)
    expert = lax.broadcasted_iota(jnp.int32, shape3, 0).reshape(slots_n, rows)
    slot = lax.broadcasted_iota(jnp.int32, shape3, 1).reshape(slots_n, rows)
    first = routes_ref[0:1, :] == expert
    second = routes_ref[1:2, :] == expert
    chosen = jnp.where(first | second, 1.0, 0.0)
    before = jnp.where(
        lax.broadcasted_iota(jnp.int32, (rows, rows), 0)
        < lax.broadcasted_iota(jnp.int32, (rows, rows), 1), 1.0, 0.0)
    rank = jnp.dot(chosen.astype(jnp.bfloat16), before.astype(jnp.bfloat16),
                   preferred_element_type=jnp.float32)
    table = jnp.where(rank == slot.astype(jnp.float32), chosen, 0.0)
    weight = jnp.where(first, gw_ref[0:1, :], 0.0) + jnp.where(second, gw_ref[1:2, :], 0.0)
    combine = (table * weight).T
    table = table.astype(jnp.bfloat16)

    tok_copy.wait()
    small[2].wait()
    values = tok[...].astype(jnp.float32)
    scale = lax.rsqrt(jnp.mean(values * values, axis=-1, keepdims=True) + 1e-06)
    for k in range(nk):
        cut = slice(k * kc, (k + 1) * kc)
        normed = (tok[:, cut].astype(jnp.float32) * scale * gain_ref[:, cut]).astype(jnp.bfloat16)
        block = jnp.dot(table, normed, preferred_element_type=jnp.float32).astype(jnp.bfloat16)
        sendbuf[k] = block.reshape(n_ep, cap, kc)
    for k in range(nk):
        recv[k, me] = sendbuf[k, me]

    pl.semaphore_wait(barrier, n_ep + jnp.where(above, 1, 0) + jnp.where(below, 1, 0))
    line_signal(0)

    dispatch = []
    for k in range(nk):
        per = []
        for i in range(1, n_ep):
            dest = lax.rem(me + i, n_ep)
            copy = pltpu.make_async_remote_copy(
                src_ref=sendbuf.at[k, dest], dst_ref=recv.at[k, me],
                send_sem=d_send.at[k, i - 1], recv_sem=d_recv.at[k, i - 1],
                device_id=(dest, t), device_id_type=MESH)
            copy.start()
            per.append(copy)
        dispatch.append(per)
    for r in range(n_z - 2):
        line_wait(r)
        line_signal(r + 1)

    for k in range(nk):
        w_copies[k][0].wait()
        w_copies[k][1].wait()
        for copy in dispatch[k]:
            copy.wait_recv()
        x = recv[k].reshape(slots_n, kc)
        g = jnp.dot(x, wg[k * kc:(k + 1) * kc, :], preferred_element_type=jnp.float32)
        u = jnp.dot(x, wu[k * kc:(k + 1) * kc, :], preferred_element_type=jnp.float32)
        if k == 0:
            acc_g[...] = g
            acc_u[...] = u
        elif k < nk - 1:
            acc_g[...] += g
            acc_u[...] += u
        else:
            g = acc_g[...] + g
            u = acc_u[...] + u
            hid[...] = (g / (1.0 + jnp.exp(-g)) * u).astype(jnp.bfloat16)

    d_copy.wait()
    order = []
    upper = 2 * z >= n_z
    for j in range(n_z - 1):
        down = n_z - 1 - j
        order.append(jnp.where(upper, jnp.where(z <= j, j + 1, j),
                               jnp.where(z >= down, down - 1, down)))
    order.append(z)
    crossing = []
    for j, zz in enumerate(order):
        cut = pl.ds(pl.multiple_of((2 * zz + other) * pw, 128), pw)
        pbuf[j] = jnp.dot(hid[...], wd[:, cut], preferred_element_type=jnp.float32)
        copy = pltpu.make_async_remote_copy(
            src_ref=pbuf.at[j], dst_ref=prbuf.at[j], send_sem=p_send.at[j], recv_sem=p_recv.at[j],
            device_id=(me, partner), device_id_type=MESH)
        copy.start()
        crossing.append(copy)
    if n_z > 1:
        line_wait(n_z - 2)
    final = []
    for j, zz in enumerate(order):
        cut = pl.ds(pl.multiple_of((2 * zz + c) * pw, 128), pw)
        own = jnp.dot(hid[...], wd[:, cut], preferred_element_type=jnp.float32)
        crossing[j].wait_recv()
        obuf[j] = (own + prbuf[j]).astype(jnp.bfloat16).reshape(n_ep, cap, pw)
        mine = j == n_z - 1
        gap = lax.rem(zz - z + n_z, n_z)
        for ds in range(n_ep - 1, -1, -1):
            dest = lax.rem(me + ds, n_ep)
            if ds or not mine:
                copy = pltpu.make_async_remote_copy(
                    src_ref=obuf.at[j, dest], dst_ref=fin.at[z, me],
                    send_sem=f_send.at[gap, ds], recv_sem=f_recv.at[gap, ds],
                    device_id=(dest, 2 * zz + c), device_id_type=MESH)
                copy.start()
                final.append(copy)
            else:
                fin[z, me] = obuf[j, me]

    for per in dispatch:
        for copy in per:
            copy.wait_send()
    for copy in crossing:
        copy.wait_send()
    for copy in final:
        copy.wait_recv()
    total = fin[0].astype(jnp.float32)
    for i in range(1, n_z):
        total = total + fin[i].astype(jnp.float32)
    mixed = jnp.dot(combine, total.reshape(slots_n, pw), precision=lax.Precision.HIGHEST,
                    preferred_element_type=jnp.float32)
    out_ref[...] = mixed.astype(jnp.bfloat16)
    for copy in final:
        copy.wait_send()


def fused(tokens, norm_gain, routes, gate_weights, expert_gate, expert_up, expert_down):
    rows, width = tokens.shape
    n_ep = lax.axis_size("ep")
    n_tp = lax.axis_size("tp")
    n_z = n_tp // 2
    pw = width // n_tp
    cap = rows // 2
    ff = expert_gate.shape[2]
    slots_n = n_ep * cap
    nk = 4
    kc = width // nk
    vmem = pl.BlockSpec(memory_space=pltpu.VMEM)
    hbm = pl.BlockSpec(memory_space=pl.ANY)
    bf, f32 = jnp.bfloat16, jnp.float32
    dma = pltpu.SemaphoreType.DMA
    return pl.pallas_call(
        functools.partial(step_kernel, n_ep, n_z, cap, nk),
        out_shape=pltpu.VMEM((rows, pw), bf),
        in_specs=[hbm] * 7,
        out_specs=vmem,
        scratch_shapes=[
            pltpu.VMEM((rows, width), bf),
            pltpu.VMEM((1, width), f32),
            pltpu.VMEM((2, rows), jnp.int32),
            pltpu.VMEM((2, rows), f32),
            pltpu.VMEM((width, ff), bf),
            pltpu.VMEM((width, ff), bf),
            pltpu.VMEM((ff, width), bf),
            pltpu.VMEM((nk, n_ep, cap, kc), bf),
            pltpu.VMEM((nk, n_ep, cap, kc), bf),
            pltpu.VMEM((slots_n, ff), f32),
            pltpu.VMEM((slots_n, ff), f32),
            pltpu.VMEM((slots_n, ff), bf),
            pltpu.VMEM((n_z, slots_n, pw), f32),
            pltpu.VMEM((n_z, slots_n, pw), f32),
            pltpu.VMEM((n_z, n_ep, cap, pw), bf),
            pltpu.VMEM((n_z, n_ep, cap, pw), bf),
            dma, dma((3,)), dma((nk,)), dma((nk,)), dma,
            dma((nk, n_ep - 1)), dma((nk, n_ep - 1)),
            dma((n_z,)), dma((n_z,)),
            dma((n_z, n_ep)), dma((n_z, n_ep)),
            pltpu.SemaphoreType.REGULAR((max(n_z - 1, 1), 2)),
        ],
        compiler_params=pltpu.CompilerParams(
            collective_id=0, has_side_effects=True, vmem_limit_bytes=60 * 1024 * 1024),
    )(tokens, norm_gain.reshape(1, width), routes.T, gate_weights.T, expert_gate, expert_up,
      expert_down)


def body(tokens, *rest):
    rows, width = tokens.shape
    n_tp = lax.axis_size("tp")
    if n_tp % 2 == 0 and (width // n_tp) % 128 == 0 and rows % 32 == 0:
        return fused(tokens, *rest)
    return shards(tokens, *rest)


def solution(mesh):
    placed = (
        P("ep", None),
        P(),
        P("ep", None),
        P("ep", None),
        P("ep", None, "tp"),
        P("ep", None, "tp"),
        P("ep", "tp", None),
    )
    return jax.shard_map(
        body, mesh=mesh, in_specs=placed, out_specs=P("ep", "tp"), check_vma=False
    )
```

```python
import functools

import jax
import jax.numpy as jnp
from jax import lax
from jax.experimental import pallas as pl
from jax.experimental.pallas import tpu as pltpu
from jax.sharding import PartitionSpec as P

MESH = pl.DeviceIdType.MESH


def expert_rows(rows, w_gate, w_up):
    gate = jnp.dot(rows, w_gate, preferred_element_type=jnp.float32)
    upper = jnp.dot(rows, w_up, preferred_element_type=jnp.float32)
    return (jax.nn.silu(gate) * upper).astype(jnp.bfloat16)


def shards(tokens, norm_gain, routes, gate_weights, expert_gate, expert_up, expert_down):
    tok_rows, width = tokens.shape
    n_ep = lax.axis_size("ep")
    n_tp = lax.axis_size("tp")
    part_width = width // n_tp
    values = tokens.astype(jnp.float32)
    scale = lax.rsqrt(jnp.mean(values * values, axis=-1, keepdims=True) + 1e-06)
    normed = (values * scale * norm_gain[None, :]).astype(jnp.bfloat16)
    w_gate = expert_gate[0]
    w_up = expert_up[0]
    w_down = expert_down[0]
    capacity = tok_rows // 2
    picks = routes.reshape(-1)
    chosen = (picks[:, None] == jnp.arange(n_ep, dtype=jnp.int32)[None, :]).astype(jnp.int32)
    ranks = jnp.cumsum(chosen, axis=0) - chosen
    place = picks * capacity + jnp.sum(ranks * chosen, axis=1)
    table = (place[None, :] == jnp.arange(n_ep * capacity, dtype=jnp.int32)[:, None]).astype(
        jnp.float32
    )
    slots = jnp.sum(table.reshape(n_ep * capacity, tok_rows, 2), axis=2)
    buffer = jnp.dot(slots.astype(jnp.bfloat16), normed, preferred_element_type=jnp.float32)
    buffer = buffer.astype(jnp.bfloat16).reshape(n_ep, capacity, width)
    combine = jnp.sum(
        (table * gate_weights.reshape(-1)[None, :]).reshape(n_ep * capacity, tok_rows, 2), axis=2
    ).T
    received = lax.all_to_all(buffer, "ep", split_axis=0, concat_axis=0, tiled=True)
    sources = received.shape[0]
    count = received.shape[1]
    hidden = expert_rows(received.reshape(sources * count, width), w_gate, w_up)
    partial_value = jnp.dot(hidden, w_down, preferred_element_type=jnp.float32)
    outputs = lax.psum_scatter(
        partial_value.reshape(sources, count, width), "tp", scatter_dimension=2, tiled=True
    )
    back = lax.all_to_all(outputs, "ep", split_axis=0, concat_axis=0, tiled=True)
    mixed = jnp.dot(
        combine,
        back.reshape(n_ep * capacity, part_width),
        precision=lax.Precision.HIGHEST,
        preferred_element_type=jnp.float32,
    )
    return mixed.astype(jnp.bfloat16)


def step_kernel(n_ep, n_z, cap, nk, tok_hbm, gain_hbm, routes_hbm, gw_hbm, wg_hbm, wu_hbm, wd_hbm,
                out_ref, tok, gain_ref, routes_ref, gw_ref, wg, wu, wd, sendbuf, recv, acc_g, acc_u,
                hid, pbuf, prbuf, obuf, fin, tok_sem, small_sem, wg_sem, wu_sem, wd_sem, d_send,
                d_recv, p_send, p_recv, f_send, f_recv, line_sem):
    me = lax.axis_index("ep")
    t = lax.axis_index("tp")
    z = t // 2
    c = t % 2
    other = 1 - c
    partner = 2 * z + other
    rows, width = tok.shape
    kc = width // nk
    pw = out_ref.shape[1]
    slots_n = n_ep * cap
    above = z < n_z - 1
    below = z > 0

    tok_copy = pltpu.make_async_copy(tok_hbm, tok, tok_sem)
    tok_copy.start()

    barrier = pltpu.get_barrier_semaphore()
    for i in range(1, n_ep):
        pl.semaphore_signal(barrier, inc=1, device_id=(lax.rem(me + i, n_ep), t),
                            device_id_type=MESH)
    pl.semaphore_signal(barrier, inc=1, device_id=(me, partner), device_id_type=MESH)

    @pl.when(above)
    def _():
        pl.semaphore_signal(barrier, inc=1, device_id=(me, t + 2), device_id_type=MESH)

    @pl.when(below)
    def _():
        pl.semaphore_signal(barrier, inc=1, device_id=(me, t - 2), device_id_type=MESH)

    def line_signal(r):
        @pl.when(above)
        def _():
            pl.semaphore_signal(line_sem.at[r, 0], inc=1, device_id=(me, t + 2),
                                device_id_type=MESH)

        @pl.when(below)
        def _():
            pl.semaphore_signal(line_sem.at[r, 1], inc=1, device_id=(me, t - 2),
                                device_id_type=MESH)

    def line_wait(r):
        @pl.when(below)
        def _():
            pl.semaphore_wait(line_sem.at[r, 0], 1)

        @pl.when(above)
        def _():
            pl.semaphore_wait(line_sem.at[r, 1], 1)

    small = [pltpu.make_async_copy(routes_hbm, routes_ref, small_sem.at[0]),
             pltpu.make_async_copy(gw_hbm, gw_ref, small_sem.at[1]),
             pltpu.make_async_copy(gain_hbm, gain_ref, small_sem.at[2])]
    for copy in small:
        copy.start()

    w_copies = []
    for k in range(nk):
        cut = pl.ds(k * kc, kc)
        cg = pltpu.make_async_copy(wg_hbm.at[0, cut], wg.at[cut], wg_sem.at[k])
        cu = pltpu.make_async_copy(wu_hbm.at[0, cut], wu.at[cut], wu_sem.at[k])
        cg.start()
        cu.start()
        w_copies.append((cg, cu))
    d_copy = pltpu.make_async_copy(wd_hbm.at[0], wd, wd_sem)
    d_copy.start()

    small[0].wait()
    small[1].wait()
    shape3 = (n_ep, cap, rows)
    expert = lax.broadcasted_iota(jnp.int32, shape3, 0).reshape(slots_n, rows)
    slot = lax.broadcasted_iota(jnp.int32, shape3, 1).reshape(slots_n, rows)
    first = routes_ref[0:1, :] == expert
    second = routes_ref[1:2, :] == expert
    chosen = jnp.where(first | second, 1.0, 0.0)
    before = jnp.where(
        lax.broadcasted_iota(jnp.int32, (rows, rows), 0)
        < lax.broadcasted_iota(jnp.int32, (rows, rows), 1), 1.0, 0.0)
    rank = jnp.dot(chosen.astype(jnp.bfloat16), before.astype(jnp.bfloat16),
                   preferred_element_type=jnp.float32)
    table = jnp.where(rank == slot.astype(jnp.float32), chosen, 0.0)
    weight = jnp.where(first, gw_ref[0:1, :], 0.0) + jnp.where(second, gw_ref[1:2, :], 0.0)
    combine = (table * weight).T
    table = table.astype(jnp.bfloat16)

    tok_copy.wait()
    small[2].wait()
    values = tok[...].astype(jnp.float32)
    scale = lax.rsqrt(jnp.mean(values * values, axis=-1, keepdims=True) + 1e-06)
    for k in range(nk):
        cut = slice(k * kc, (k + 1) * kc)
        normed = (tok[:, cut].astype(jnp.float32) * scale * gain_ref[:, cut]).astype(jnp.bfloat16)
        block = jnp.dot(table, normed, preferred_element_type=jnp.float32).astype(jnp.bfloat16)
        sendbuf[k] = block.reshape(n_ep, cap, kc)
    for k in range(nk):
        recv[k, me] = sendbuf[k, me]

    pl.semaphore_wait(barrier, n_ep + jnp.where(above, 1, 0) + jnp.where(below, 1, 0))

    dispatch = []
    for k in range(nk):
        per = []
        for i in range(1, n_ep):
            dest = lax.rem(me + i, n_ep)
            copy = pltpu.make_async_remote_copy(
                src_ref=sendbuf.at[k, dest], dst_ref=recv.at[k, me],
                send_sem=d_send.at[k, i - 1], recv_sem=d_recv.at[k, i - 1],
                device_id=(dest, t), device_id_type=MESH)
            copy.start()
            per.append(copy)
        dispatch.append(per)
    line_signal(0)
    for r in range(n_z - 2):
        line_wait(r)
        line_signal(r + 1)

    for k in range(nk):
        w_copies[k][0].wait()
        w_copies[k][1].wait()
        for copy in dispatch[k]:
            copy.wait_recv()
        x = recv[k].reshape(slots_n, kc)
        g = jnp.dot(x, wg[k * kc:(k + 1) * kc, :], preferred_element_type=jnp.float32)
        u = jnp.dot(x, wu[k * kc:(k + 1) * kc, :], preferred_element_type=jnp.float32)
        if nk == 1:
            hid[...] = (g / (1.0 + jnp.exp(-g)) * u).astype(jnp.bfloat16)
        elif k == 0:
            acc_g[...] = g
            acc_u[...] = u
        elif k < nk - 1:
            acc_g[...] += g
            acc_u[...] += u
        else:
            g = acc_g[...] + g
            u = acc_u[...] + u
            hid[...] = (g / (1.0 + jnp.exp(-g)) * u).astype(jnp.bfloat16)

    d_copy.wait()
    order = []
    upper = 2 * z >= n_z
    for j in range(n_z - 1):
        down = n_z - 1 - j
        order.append(jnp.where(upper, jnp.where(z <= j, j + 1, j),
                               jnp.where(z >= down, down - 1, down)))
    order.append(z)
    crossing = []
    for j, zz in enumerate(order):
        cut = pl.ds(pl.multiple_of((2 * zz + other) * pw, 128), pw)
        pbuf[j] = jnp.dot(hid[...], wd[:, cut], preferred_element_type=jnp.float32)
        copy = pltpu.make_async_remote_copy(
            src_ref=pbuf.at[j], dst_ref=prbuf.at[j], send_sem=p_send.at[j], recv_sem=p_recv.at[j],
            device_id=(me, partner), device_id_type=MESH)
        copy.start()
        crossing.append(copy)
    if n_z > 1:
        line_wait(n_z - 2)
    final = []
    for j, zz in enumerate(order):
        cut = pl.ds(pl.multiple_of((2 * zz + c) * pw, 128), pw)
        own = jnp.dot(hid[...], wd[:, cut], preferred_element_type=jnp.float32)
        crossing[j].wait_recv()
        obuf[j] = (own + prbuf[j]).astype(jnp.bfloat16).reshape(n_ep, cap, pw)
        mine = j == n_z - 1
        gap = lax.rem(zz - z + n_z, n_z)
        for ds in range(n_ep - 1, -1, -1):
            dest = lax.rem(me + ds, n_ep)
            if ds or not mine:
                copy = pltpu.make_async_remote_copy(
                    src_ref=obuf.at[j, dest], dst_ref=fin.at[z, me],
                    send_sem=f_send.at[gap, ds], recv_sem=f_recv.at[gap, ds],
                    device_id=(dest, 2 * zz + c), device_id_type=MESH)
                copy.start()
                final.append(copy)
            else:
                fin[z, me] = obuf[j, me]

    for per in dispatch:
        for copy in per:
            copy.wait_send()
    for copy in crossing:
        copy.wait_send()
    for copy in final:
        copy.wait_recv()
    total = fin[0].astype(jnp.float32)
    for i in range(1, n_z):
        total = total + fin[i].astype(jnp.float32)
    mixed = jnp.dot(combine, total.reshape(slots_n, pw), precision=lax.Precision.HIGHEST,
                    preferred_element_type=jnp.float32)
    out_ref[...] = mixed.astype(jnp.bfloat16)
    for copy in final:
        copy.wait_send()


def fused(tokens, norm_gain, routes, gate_weights, expert_gate, expert_up, expert_down):
    rows, width = tokens.shape
    n_ep = lax.axis_size("ep")
    n_tp = lax.axis_size("tp")
    n_z = n_tp // 2
    pw = width // n_tp
    cap = rows // 2
    ff = expert_gate.shape[2]
    slots_n = n_ep * cap
    nk = 2
    kc = width // nk
    vmem = pl.BlockSpec(memory_space=pltpu.VMEM)
    hbm = pl.BlockSpec(memory_space=pl.ANY)
    bf, f32 = jnp.bfloat16, jnp.float32
    dma = pltpu.SemaphoreType.DMA
    return pl.pallas_call(
        functools.partial(step_kernel, n_ep, n_z, cap, nk),
        out_shape=pltpu.VMEM((rows, pw), bf),
        in_specs=[hbm] * 7,
        out_specs=vmem,
        scratch_shapes=[
            pltpu.VMEM((rows, width), bf),
            pltpu.VMEM((1, width), f32),
            pltpu.VMEM((2, rows), jnp.int32),
            pltpu.VMEM((2, rows), f32),
            pltpu.VMEM((width, ff), bf),
            pltpu.VMEM((width, ff), bf),
            pltpu.VMEM((ff, width), bf),
            pltpu.VMEM((nk, n_ep, cap, kc), bf),
            pltpu.VMEM((nk, n_ep, cap, kc), bf),
            pltpu.VMEM((slots_n, ff), f32),
            pltpu.VMEM((slots_n, ff), f32),
            pltpu.VMEM((slots_n, ff), bf),
            pltpu.VMEM((n_z, slots_n, pw), f32),
            pltpu.VMEM((n_z, slots_n, pw), f32),
            pltpu.VMEM((n_z, n_ep, cap, pw), bf),
            pltpu.VMEM((n_z, n_ep, cap, pw), bf),
            dma, dma((3,)), dma((nk,)), dma((nk,)), dma,
            dma((nk, n_ep - 1)), dma((nk, n_ep - 1)),
            dma((n_z,)), dma((n_z,)),
            dma((n_z, n_ep)), dma((n_z, n_ep)),
            pltpu.SemaphoreType.REGULAR((max(n_z - 1, 1), 2)),
        ],
        compiler_params=pltpu.CompilerParams(
            collective_id=0, has_side_effects=True, vmem_limit_bytes=60 * 1024 * 1024),
    )(tokens, norm_gain.reshape(1, width), routes.T, gate_weights.T, expert_gate, expert_up,
      expert_down)


def body(tokens, *rest):
    rows, width = tokens.shape
    n_tp = lax.axis_size("tp")
    if n_tp % 2 == 0 and (width // n_tp) % 128 == 0 and rows % 32 == 0:
        return fused(tokens, *rest)
    return shards(tokens, *rest)


def solution(mesh):
    placed = (
        P("ep", None),
        P(),
        P("ep", None),
        P("ep", None),
        P("ep", None, "tp"),
        P("ep", None, "tp"),
        P("ep", "tp", None),
    )
    return jax.shard_map(
        body, mesh=mesh, in_specs=placed, out_specs=P("ep", "tp"), check_vma=False
    )
```
